32 devices in a mesh: kv: 16 (over z, y, x), tp: 2 (over core).
Axes of the slice: x: 2, y: 2, z: 4, core: 2. Of those that a mesh axis runs over, the one named last changes fastest.
Arguments:
- tokens: bfloat16 [32, 4096], P(None, 'kv'), may hold values from -16 to 16
- mix_gain: bfloat16 [4096], P('kv'), may hold values from 0.099609375 to 1.8984375
- ffn_gain: bfloat16 [4096], P('kv'), may hold values from 0.099609375 to 1.8984375
- w_query: bfloat16 [4096, 2048], P('kv', 'tp'), may hold values from -0.09375 to 0.09375
- w_key: bfloat16 [4096, 2048], P('kv', 'tp'), may hold values from -0.09375 to 0.09375
- w_value: bfloat16 [4096, 4096], P('kv', 'tp'), may hold values from -0.09375 to 0.09375
- w_gate: bfloat16 [4096, 4096], P('kv', 'tp'), may hold values from -0.09375 to 0.09375
- w_decay: bfloat16 [4096, 2048], P('kv', 'tp'), may hold values from -0.375 to 0.375
- decay_bias: float32 [2048], P('tp'), may hold values from -7 to 4
- head_gain: bfloat16 [512], replicated, may hold values from 0.099609375 to 1.8984375
- w_output: bfloat16 [4096, 4096], P('tp', 'kv'), may hold values from -0.09375 to 0.09375
- w_ffgate: bfloat16 [4096, 11008], P('kv', 'tp'), may hold values from -0.09375 to 0.09375
- w_ffup: bfloat16 [4096, 11008], P('kv', 'tp'), may hold values from -0.09375 to 0.09375
- w_down: bfloat16 [11008, 4096], P('tp', 'kv'), may hold values from -0.0546875 to 0.0546875
- state: float32 [32, 8, 256, 512], P('kv', 'tp'), may hold values from -6 to 6
Outputs:
- mixed: bfloat16 [32, 4096], P(None, 'kv')
- new_state: float32 [32, 8, 256, 512], P('kv', 'tp')
The draws below stay inside these ranges and needn't reach their ends.
All inputs are finite; a program needn't handle non-finite values.
Results may differ from the reference program's by a relative error of at most 0.015.
Values may be sent and summed in bfloat16 or wider, within the bound.
No kernel may reach another device: no remote copies, remote signals or barrier semaphores. Data moves between devices by JAX's collectives and lax.ppermute only.
A program may use at most 64 MiB of HBM per device.

```python
import jax
import jax.numpy as jnp
from jax import lax

D = 4096
HEADS = 8
DK = 256
DV = 512
FF = 11008
SEQS = 32
GROUPS = 2


def draw_tokens(key, part):
    column = jnp.arange(D, dtype=jnp.float32) / D
    column_scale = 0.4 * jnp.exp(jnp.log(6.0) * column)
    values = jnp.clip(jax.random.normal(key, (SEQS, D), jnp.float32), -4.0, 4.0) * column_scale
    return values.astype(jnp.bfloat16)


def shard_levels(key, dims, pieces, least, largest):
    def one(dim, parts):
        steps = jax.random.uniform(jax.random.fold_in(jax.random.fold_in(key, 6), dim), (parts,), jnp.float32, least / len(pieces), largest / len(pieces))
        return jnp.repeat(jnp.exp(steps), dims[dim] // parts).reshape((-1,) + (1,) * (len(dims) - dim - 1))

    factor_of = one(*pieces[0])
    for cut in pieces[1:]:
        factor_of = factor_of * one(*cut)
    return factor_of


def normal_values(stream_key, extent, scale, reach, cuts=(), kind=jnp.bfloat16):
    values = jax.random.normal(stream_key, extent, jnp.float32) * scale
    if len(cuts) > 0:
        values = shard_levels(stream_key, extent, cuts, -0.22, 0.18) * values
    return jnp.clip(values, min=-reach, max=reach).astype(kind)


def setup_inputs(seed: int = 0) -> dict:
    key_of = jax.random.split(jax.random.key(seed), 16)
    tokens = draw_tokens(jax.random.fold_in(key_of[15], 71), 0)
    mix_gain = jnp.clip(1.0 + 0.18 * jax.random.normal(key_of[1], (D,), jnp.float32), 0.099609375, 1.8984375).astype(jnp.bfloat16)
    ffn_gain = jnp.clip(1.0 + 0.18 * jax.random.normal(key_of[2], (D,), jnp.float32), 0.099609375, 1.8984375).astype(jnp.bfloat16)
    w_query = normal_values(key_of[3], (D, HEADS * DK), D ** -0.5, 0.09375, ((0, 16), (1, 2)))
    w_key = normal_values(key_of[4], (D, HEADS * DK), D ** -0.5, 0.09375, ((0, 16), (1, 2)))
    w_value = normal_values(key_of[5], (D, HEADS * DV), D ** -0.5, 0.09375, ((0, 16), (1, 2)))
    w_gate = normal_values(key_of[6], (D, HEADS * DV), D ** -0.5, 0.09375, ((0, 16), (1, 2)))
    w_decay = normal_values(key_of[7], (D, HEADS * DK), (D // 16) ** -0.5, 0.375, ((0, 16), (1, 2)))
    decay_bias = jnp.clip(-7.0 + 11.0 * jax.random.uniform(key_of[8], (HEADS * DK,), jnp.float32) ** shard_levels(key_of[8], (HEADS * DK,), ((0, 2),), -0.2, 0.2), -7.0, 4.0)
    head_gain = jnp.clip(1.0 + 0.18 * jax.random.normal(key_of[9], (DV,), jnp.float32), 0.099609375, 1.8984375).astype(jnp.bfloat16)
    w_output = normal_values(key_of[10], (HEADS * DV, D), (HEADS * DV) ** -0.5, 0.09375, ((0, 2), (1, 16)))
    w_ffgate = normal_values(key_of[11], (D, FF), D ** -0.5, 0.09375, ((0, 16), (1, 2)))
    w_ffup = normal_values(key_of[12], (D, FF), D ** -0.5, 0.09375, ((0, 16), (1, 2)))
    w_down = normal_values(key_of[13], (FF, D), FF ** -0.5, 0.0546875, ((0, 2), (1, 16)))
    state = normal_values(key_of[14], (SEQS, HEADS, DK, DV), 1.0, 6.0, ((0, 16), (1, 2)), jnp.float32)
    return {"tokens": tokens, "mix_gain": mix_gain, "ffn_gain": ffn_gain, "w_query": w_query, "w_key": w_key, "w_value": w_value, "w_gate": w_gate, "w_decay": w_decay, "decay_bias": decay_bias, "head_gain": head_gain, "w_output": w_output, "w_ffgate": w_ffgate, "w_ffup": w_ffup, "w_down": w_down, "state": state}


epsilon = 1e-06

def reference(tokens, mix_gain, ffn_gain, w_query, w_key, w_value, w_gate, w_decay, decay_bias, head_gain, w_output, w_ffgate, w_ffup, w_down, state):
    seq_count = tokens.shape[0]
    model_width = tokens.shape[1]
    head_count = state.shape[1]
    key_dim = state.shape[2]
    val_dim = state.shape[3]
    token_f32 = tokens.astype(jnp.float32)
    mix_rms = lax.rsqrt(lax.optimization_barrier(jnp.sum(token_f32 * token_f32, axis=1)) / model_width + epsilon)[:, None]
    mix_in = (token_f32 * mix_gain.astype(jnp.float32)).astype(jnp.bfloat16)

    def project(weight):
        return jnp.dot(mix_in, weight, preferred_element_type=jnp.float32) * mix_rms
    queries = project(w_query).reshape(seq_count, head_count, key_dim) * key_dim ** (-0.5)
    key_rows = project(w_key).reshape(seq_count, head_count, key_dim)
    value_rows = project(w_value).reshape(seq_count, head_count, val_dim)
    gate_rows = project(w_gate).reshape(seq_count, head_count, val_dim)
    decay_rows = (project(w_decay) + decay_bias).reshape(seq_count, head_count, key_dim)
    log_decay = jax.nn.log_sigmoid(decay_rows) / 16.0
    new_state = jnp.exp(log_decay)[..., None] * state + key_rows[..., :, None] * value_rows[..., None, :]
    attended = jnp.einsum('bhk,bhkv->bhv', queries, new_state, precision=lax.Precision.HIGHEST)
    attended = attended * lax.rsqrt(lax.optimization_barrier(jnp.sum(attended * attended, axis=2, keepdims=True)) / val_dim + epsilon)
    head_out = (attended * head_gain.astype(jnp.float32) * jax.nn.silu(gate_rows)).reshape(seq_count, head_count * val_dim).astype(jnp.bfloat16)
    group_cols = head_count * val_dim // GROUPS
    attn_out = jnp.zeros((seq_count, model_width), jnp.float32)
    for group_idx in range(GROUPS):
        partial_value = jnp.dot(head_out[:, group_idx * group_cols:(group_idx + 1) * group_cols], w_output[group_idx * group_cols:(group_idx + 1) * group_cols], preferred_element_type=jnp.float32)
        attn_out = attn_out + lax.optimization_barrier(partial_value.astype(jnp.bfloat16)).astype(jnp.float32)
    residual_mid = (token_f32 + attn_out).astype(jnp.bfloat16)
    mid_f32 = residual_mid.astype(jnp.float32)
    ffn_rms = lax.rsqrt(lax.optimization_barrier(jnp.sum(mid_f32 * mid_f32, axis=1)) / model_width + epsilon)[:, None]
    ffn_in = (mid_f32 * ffn_gain.astype(jnp.float32)).astype(jnp.bfloat16)
    gate_sum = jnp.dot(ffn_in, w_ffgate, preferred_element_type=jnp.float32)
    up_sum = jnp.dot(ffn_in, w_ffup, preferred_element_type=jnp.float32)
    hidden = (jax.nn.silu(gate_sum * ffn_rms) * (up_sum * ffn_rms)).astype(jnp.bfloat16)
    unit_cols = hidden.shape[1] // GROUPS
    ffn_out = jnp.zeros((seq_count, model_width), jnp.float32)
    for group_idx in range(GROUPS):
        partial_value = jnp.dot(hidden[:, group_idx * unit_cols:(group_idx + 1) * unit_cols], w_down[group_idx * unit_cols:(group_idx + 1) * unit_cols], preferred_element_type=jnp.float32)
        ffn_out = ffn_out + lax.optimization_barrier(partial_value.astype(jnp.bfloat16)).astype(jnp.float32)
    mixed = (mid_f32 + ffn_out).astype(jnp.bfloat16)
    return (mixed, new_state)
```

```python
import functools

import jax
import jax.numpy as jnp
from jax import lax
from jax.experimental import pallas as pl
from jax.experimental.pallas import tpu as pltpu
from jax.sharding import PartitionSpec as P


epsilon = 1e-06
f32 = jnp.float32
bf16 = jnp.bfloat16
LANES = 128
VMEM = pl.BlockSpec(memory_space=pltpu.VMEM)
HBM = pl.BlockSpec(memory_space=pltpu.HBM)


def exchange(value, axis, size, mask):
    return lax.ppermute(value, axis, [(i, i ^ mask) for i in range(size)])


def padded(width):
    return -(-width // LANES) * LANES


def call(body, outs, operands, flops, read, scratch=(), specs=None, vmem=16 << 20, out_specs=None):
    if specs:
        operands = [pltpu.with_memory_space_constraint(x, pltpu.HBM) if spec is HBM else x for x, spec in zip(operands, specs)]
    return pl.pallas_call(
        body,
        out_shape=[jax.ShapeDtypeStruct(shape, dtype) for shape, dtype in outs],
        in_specs=specs or [VMEM] * len(operands),
        out_specs=out_specs or [VMEM] * len(outs),
        scratch_shapes=list(scratch),
        cost_estimate=pl.CostEstimate(flops=flops, bytes_accessed=read, transcendentals=0),
        compiler_params=pltpu.CompilerParams(vmem_limit_bytes=vmem),
    )(*operands)


def store_squares(values, parts, at):
    sums = jnp.sum(values * values, axis=1, keepdims=True)
    high = sums.astype(bf16).astype(f32)
    lane = lax.broadcasted_iota(jnp.int32, (values.shape[0], LANES), 1)
    tail = jnp.where(lane == 0, high, jnp.where(lane == 1, sums - high, 0.0)).astype(bf16)
    rows = parts[0].shape[0]
    for s, part in enumerate(parts):
        part[:, at:at + LANES] = tail[s * rows:(s + 1) * rows]


def store_product(left, weight, parts, at, step=512):
    rows = parts[0].shape[0]
    width = weight.shape[1]
    for low in range(0, width, step):
        high = min(width, low + step)
        product = jnp.dot(left, weight[:, low:high], preferred_element_type=f32).astype(bf16)
        for s, part in enumerate(parts):
            part[:, at + low:at + high] = product[s * rows:(s + 1) * rows]
    if padded(width) > width:
        for part in parts:
            part[:, at + width:at + padded(width)] = jnp.zeros((rows, padded(width) - width), bf16)


def project_kernel(inner, perm, *refs):
    sources, refs = refs[:7], refs[7:]
    ordered, parts, refs = refs[0], refs[1:1 + inner], refs[1 + inner:]
    held, sems = refs[:7], refs[7]
    copies = [pltpu.make_async_copy(w, h, sems.at[i]) for i, (w, h) in enumerate(zip(sources, held))]
    for copy in copies:
        copy.start()
    copies[0].wait()
    copies[1].wait()
    token_f32 = jnp.dot(perm[...], held[0][...], preferred_element_type=f32)
    ordered[...] = token_f32.astype(bf16)
    mix_in = (token_f32 * held[1][...].astype(f32).reshape(1, -1)).astype(bf16)
    at = 0
    store_squares(token_f32, parts, sum(padded(w.shape[1]) for w in held[2:]))
    for copy, h in zip(copies[2:], held[2:]):
        copy.wait()
        store_product(mix_in, h, parts, at)
        at += padded(h.shape[1])


def attend_kernel(own, heads, key_dim, val_dim, width, bias, gain, state, *refs):
    pieces, (out, turned, values, rows, flat) = refs[:-5], refs[-5:]
    total = pieces[0][...].astype(f32)
    for piece in pieces[1:]:
        total = total + piece[...].astype(f32)
    keys, vals = heads * key_dim, heads * val_dim
    at_key, at_value = padded(keys), 2 * padded(keys)
    at_gate = at_value + padded(vals)
    at_decay = at_gate + padded(vals)
    at_squares = at_decay + padded(keys)
    squares = total[:, at_squares:at_squares + 1] + total[:, at_squares + 1:at_squares + 2]
    rms = lax.rsqrt(squares / width + epsilon)
    query = total[:, :keys] * rms * key_dim ** (-0.5)
    key = total[:, at_key:at_key + keys] * rms
    value = total[:, at_value:at_value + vals] * rms
    gate = total[:, at_gate:at_gate + vals] * rms
    pre = total[:, at_decay:at_decay + keys] * rms + bias[...]
    log_decay = -(jnp.maximum(-pre, 0.0) + jnp.log1p(jnp.exp(-jnp.abs(pre)))) / 16.0
    decay = jnp.exp(log_decay)
    scaled = query * decay
    gated = gate / (1.0 + jnp.exp(-gate))
    product = query * key
    count = own * heads
    rows[...] = jnp.zeros_like(rows)
    for b in range(own):
        for h in range(heads):
            i = b * heads + h
            cut = slice(h * key_dim, (h + 1) * key_dim)
            rows[i:i + 1, :] = scaled[b:b + 1, cut]
            rows[count + i:count + i + 1, :] = decay[b:b + 1, cut]
            rows[2 * count + i:2 * count + i + 1, :] = key[b:b + 1, cut]
            values[i:i + 1, :] = value[b:b + 1, h * val_dim:(h + 1) * val_dim]
    columns = jnp.transpose(rows[...])
    turned[...] = columns
    for b in range(own):
        for h in range(heads):
            i = b * heads + h
            cut = slice(h * val_dim, (h + 1) * val_dim)
            dot = jnp.sum(product[b:b + 1, h * key_dim:(h + 1) * key_dim], axis=1, keepdims=True)
            attended = jnp.sum(columns[:, i:i + 1] * state[b, h], axis=0, keepdims=True) + dot * value[b:b + 1, cut]
            scale = lax.rsqrt(jnp.sum(attended * attended, axis=1, keepdims=True) / val_dim + epsilon)
            flat[b:b + 1, cut] = attended * scale * gain[...].astype(f32) * gated[b:b + 1, cut]
    out[...] = flat[...].astype(bf16)


def fetch_kernel(state, weight, state_out, weight_out, sems):
    count, depth = state.shape[0], weight.shape[0] // 2
    copies = [pltpu.make_async_copy(state.at[b, h], state_out.at[b, h], sems.at[b * state.shape[1] + h])
              for b in range(count) for h in range(state.shape[1])]
    last = len(copies)
    copies += [pltpu.make_async_copy(weight.at[pl.ds(i * depth, depth)], weight_out.at[pl.ds(i * depth, depth)], sems.at[last + i])
               for i in range(2)]
    for copy in copies:
        copy.start()
    for copy in copies:
        copy.wait()


def state_kernel(own, heads, turned, values, state, new_state, held, sems):
    count = own * heads
    copies = []
    for b in range(own):
        for h in range(heads):
            i = b * heads + h
            decay = turned[:, count + i:count + i + 1]
            key = turned[:, 2 * count + i:2 * count + i + 1]
            held[b, h] = decay * state[b, h] + key * values[i:i + 1, :]
            copies.append(pltpu.make_async_copy(held.at[b, h], new_state.at[b, h], sems.at[i]))
            copies[-1].start()
    for copy in copies:
        copy.wait()


def multiply_kernel(weight, *refs):
    left, out = refs[:-1], refs[-1]
    rows = jnp.concatenate([ref[...] for ref in left], axis=0)
    out[...] = jnp.dot(rows, weight[...], preferred_element_type=f32).astype(bf16)


def ffn_kernel(groups, tokens, gain, gate, up, *refs):
    partials, middle, parts = refs[:groups], refs[groups], refs[groups + 1:]
    total = partials[0][...].astype(f32)
    for partial in partials[1:]:
        total = total + partial[...].astype(f32)
    middle[...] = (tokens[...].astype(f32) + total).astype(bf16)
    mid = middle[...].astype(f32)
    ffn_in = (mid * gain[...].astype(f32)).astype(bf16)
    units = padded(gate.shape[1])
    store_squares(mid, parts, 2 * units)
    store_product(ffn_in, gate, parts, 0)
    store_product(ffn_in, up, parts, units)


def hidden_kernel(units, width, *refs):
    pieces, out = refs[:-1], refs[-1]
    total = pieces[0][...].astype(f32)
    for piece in pieces[1:]:
        total = total + piece[...].astype(f32)
    at = padded(units)
    squares = total[:, 2 * at:2 * at + 1] + total[:, 2 * at + 1:2 * at + 2]
    rms = lax.rsqrt(squares / width + epsilon)
    gate = total[:, :units] * rms
    out[...] = (gate / (1.0 + jnp.exp(-gate)) * (total[:, at:at + units] * rms)).astype(bf16)


def final_kernel(perm, middle, *refs):
    partials, out = refs[:-1], refs[-1]
    total = partials[0][...].astype(f32)
    for partial in partials[1:]:
        total = total + partial[...].astype(f32)
    mixed = (middle[...].astype(f32) + total).astype(bf16)
    back = lax.dot_general(perm[...], mixed, (((0,), (0,)), ((), ())), preferred_element_type=f32)
    out[...] = back.astype(bf16)


def reduce_rows(parts, size, inner):
    outer = size // inner
    sent = [exchange(parts[s], "kv", size, s) for s in range(1, inner)]
    total = parts[0].astype(f32)
    for value in sent:
        total = total + value.astype(f32)
    blocks = total.astype(bf16).reshape(outer, total.shape[0] // outer, total.shape[1])
    return [blocks[0]] + [exchange(blocks[u], "kv", size, u * inner) for u in range(1, outer)]


def gather_rows(rows, size, inner):
    outer = size // inner
    sent = [exchange(rows, "kv", size, u * inner) for u in range(1, outer)]
    rows = jnp.concatenate([rows] + sent, 0)
    return [rows] + [exchange(rows, "kv", size, s) for s in range(1, inner)]


def over_tp(part, size):
    return [part] + [exchange(part, "tp", size, mask) for mask in range(1, size)]


def local(size, groups, inner, tokens, mix_gain, ffn_gain, w_query, w_key, w_value, w_gate, w_decay, decay_bias, head_gain,
          w_output, w_ffgate, w_ffup, w_down, state):
    own, heads, key_dim, val_dim = state.shape
    seqs, channels = tokens.shape
    width = channels * size
    outer = size // inner
    index = jnp.arange(seqs, dtype=jnp.int32)
    block = index // own
    source = ((block // outer + block % outer * inner) ^ lax.axis_index("kv")) * own + index % own
    perm = (source[:, None] == index[None, :]).astype(bf16)

    weights = (w_query, w_key, w_value, w_gate, w_decay)
    total = sum(padded(w.shape[1]) for w in weights) + LANES
    rows = seqs // inner
    ordered, *parts = call(
        functools.partial(project_kernel, inner),
        [((seqs, channels), bf16)] + [((rows, total), bf16)] * inner,
        (perm, tokens, mix_gain, *weights),
        2 * seqs * channels * total, 2 * channels * total,
        scratch=[pltpu.VMEM(w.shape, bf16) for w in (tokens, mix_gain, *weights)] + [pltpu.SemaphoreType.DMA((7,))],
        specs=[VMEM] + [HBM] * 7,
    )
    held_state, held_output = call(
        fetch_kernel, [(state.shape, f32), (w_output.shape, bf16)], (state, w_output),
        0, 4 * state.size + 2 * w_output.size,
        scratch=[pltpu.SemaphoreType.DMA((own * heads + 2,))], specs=[HBM] * 2, vmem=1 << 20,
    )
    pieces = reduce_rows(parts, size, inner)
    count = own * heads
    deep = -(-3 * count // 8) * 8
    head_out, turned, values = call(
        functools.partial(attend_kernel, own, heads, key_dim, val_dim, width),
        [((own, heads * val_dim), bf16), ((key_dim, deep), f32), ((count, val_dim), f32)],
        (decay_bias.reshape(1, -1), head_gain.reshape(1, -1), held_state, *pieces),
        4 * state.size, 4 * state.size,
        scratch=[pltpu.VMEM((deep, key_dim), f32), pltpu.VMEM((own, heads * val_dim), f32)],
    )
    new_state, = call(
        functools.partial(state_kernel, own, heads), [(state.shape, f32)], (turned, values, held_state),
        4 * state.size, 8 * state.size,
        scratch=[pltpu.VMEM(state.shape, f32), pltpu.SemaphoreType.DMA((count,))],
        out_specs=[HBM],
    )
    gathered = gather_rows(head_out, size, inner)
    partial, = call(multiply_kernel, [((seqs, channels), bf16)], (held_output, *gathered),
                    2 * seqs * w_output.size, 2 * w_output.size)
    units = w_ffgate.shape[1]
    middle, *parts = call(
        functools.partial(ffn_kernel, groups),
        [((seqs, channels), bf16)] + [((rows, 2 * padded(units) + LANES), bf16)] * inner,
        (ordered, ffn_gain.reshape(1, -1), w_ffgate, w_ffup, *over_tp(partial, groups)),
        4 * seqs * w_ffgate.size, 4 * w_ffgate.size,
    )
    pieces = reduce_rows(parts, size, inner)
    hidden, = call(functools.partial(hidden_kernel, units, width), [((own, units), bf16)], pieces,
                   32 * own * units, 8 * own * units)
    gathered = gather_rows(hidden, size, inner)
    partial, = call(multiply_kernel, [((seqs, channels), bf16)], (w_down, *gathered),
                    2 * seqs * w_down.size, 2 * w_down.size)
    mixed, = call(final_kernel, [((seqs, channels), bf16)], (perm, middle, *over_tp(partial, groups)),
                  4 * seqs * channels, 8 * seqs * channels)
    return (mixed, new_state)


def solution(mesh):
    size, groups = mesh.shape["kv"], mesh.shape["tp"]
    if size & (size - 1) or groups & (groups - 1):
        raise ValueError("axis sizes")
    inner = 1 << ((size.bit_length() - 1) // 2)
    rows, columns = P("tp", "kv"), P("kv", "tp")
    in_specs = (P(None, "kv"), P("kv"), P("kv"), columns, columns, columns, columns, columns, P("tp"), P(), rows, columns, columns,
                rows, P("kv", "tp", None, None))
    out_specs = (P(None, "kv"), P("kv", "tp", None, None))

    def body(*args):
        return local(size, groups, inner, *args)

    return jax.shard_map(body, mesh=mesh, in_specs=in_specs, out_specs=out_specs, check_vma=False)
```
